32 devices in a mesh: kv: 8 (over z, y), tp: 4 (over x, core).
Axes of the slice: x: 2, y: 2, z: 4, core: 2. Of those that a mesh axis runs over, the one named last changes fastest.
Arguments:
- inputs: bfloat16 [4096, 2048], P('kv'), may hold values from -128 to 128
- w_query: bfloat16 [2048, 2048], P(None, 'tp'), may hold values from -0.125 to 0.125
- w_key: bfloat16 [2048, 1024], P(None, 'tp'), may hold values from -0.125 to 0.125
- w_value: bfloat16 [2048, 1024], P(None, 'tp'), may hold values from -0.125 to 0.125
- w_out: bfloat16 [2048, 2048], P(None, 'tp'), may hold values from -0.125 to 0.125
- chosen: int32 [128, 8], P('kv'), may hold values from -1 to 127, as said below
Outputs:
- mixed: bfloat16 [4096, 2048], P('kv', 'tp')
- log_total: float32 [16, 4096], P('tp', 'kv')
The draws below stay inside these ranges and needn't reach their ends.
Inputs may be any that keep to these rules, and one draw needn't show every extreme that they name: `chosen`: row i has entry 0 equal to i. Rows 16 * r to 16 * r + 15 belong to index r of kv. For k from 1 to 7, entry k of these rows is -1 or one and the same block held by index r - d, with d = 1 + (k - 1) * 1; it is -1 in all of them where r - d is negative, and the last of these rows lists every such block that exists.
All inputs are finite; a program needn't handle non-finite values.
Results may differ from the reference program's by a relative error of at most 0.015.
Values may be sent and summed in bfloat16 or wider, within the bound.
A program may use at most 192 MiB of HBM per device.

```python
import jax
import jax.numpy as jnp
from jax import lax

D = 2048
HEADS = 16
KV_HEADS = 8
HD = 128
BLK = 32
SEL = 8
NB_DEV = 16
TOKENS = 4096
NBLOCKS = 128
N_KV = 8


def draw_inputs(key, part):
    base = jnp.clip(jax.random.normal(key, (TOKENS, D), jnp.float32), -6.0, 6.0)
    return base.astype(jnp.bfloat16)


def draw_chosen(key, part):
    key_inner = jax.random.fold_in(key, 13)
    key_rows = jax.random.fold_in(key, 14)
    count = SEL - 1
    reaches = jnp.array([1 + column * (N_KV - 2) // (count - 1) for column in range(count)], jnp.int32)
    reader = jnp.arange(N_KV, dtype=jnp.int32)[:, None]
    owner = reader - reaches[None, :]
    present = owner >= 0
    inner = jax.random.randint(key_inner, (N_KV, count), 0, NB_DEV)
    block = owner * NB_DEV + inner
    rows = jnp.arange(NB_DEV, dtype=jnp.int32)
    keep = jax.random.randint(key_rows, (N_KV, NB_DEV, count), 0, 4) != 0
    keep = keep | (rows[None, :, None] == NB_DEV - 1)
    rest = jnp.where(present[:, None, :] & keep, block[:, None, :], -1)
    own = reader * NB_DEV + rows[None, :]
    return jnp.concatenate([own[..., None], rest], axis=-1).reshape(N_KV * NB_DEV, SEL).astype(jnp.int32)


def shard_levels(stream_key, shape, shards, low, high):
    def one(axis_at, shards_of):
        draws = jax.random.uniform(jax.random.fold_in(jax.random.fold_in(stream_key, 6), axis_at), (shards_of,), jnp.float32, low / len(shards), high / len(shards))
        return jnp.repeat(jnp.exp(draws), shape[axis_at] // shards_of).reshape((-1,) + (1,) * (len(shape) - axis_at - 1))

    loudness = one(*shards[0])
    for cut in shards[1:]:
        loudness = loudness * one(*cut)
    return loudness


def centred(stream_key, extent, width, most, shards=(), kind=jnp.bfloat16):
    values = width * jax.random.normal(stream_key, extent, jnp.float32)
    if shards:
        values = values * shard_levels(stream_key, extent, shards, -0.22, 0.18)
    return jnp.clip(values, -most, most).astype(kind)


def setup_inputs(seed: int = 0) -> dict:
    key_of = jax.random.split(jax.random.key(seed), 7)
    inputs = draw_inputs(jax.random.fold_in(key_of[6], 71), 0)
    w_query = centred(key_of[1], (D, HEADS * HD), D ** -0.5, 0.125, ((1, 4),))
    w_key = centred(key_of[2], (D, KV_HEADS * HD), D ** -0.5, 0.125, ((1, 4),))
    w_value = centred(key_of[3], (D, KV_HEADS * HD), D ** -0.5, 0.125, ((1, 4),))
    w_out = centred(key_of[4], (HEADS * HD, D), (HEADS * HD) ** -0.5, 0.125, ((1, 4),))
    chosen = draw_chosen(jax.random.fold_in(key_of[6], 71), 0)
    return dict(inputs=inputs, w_query=w_query, w_key=w_key, w_value=w_value, w_out=w_out, chosen=chosen)


def rotate(tensor, positions):
    half = tensor.shape[-1] // 2
    inverse = 10000.0 ** (-jnp.arange(0, 2 * half, 2, dtype=jnp.float32) / (2 * half))
    angles = positions.astype(jnp.float32)[:, None] * inverse[None, :]
    cosine = jnp.cos(angles)[:, None, :]
    sine = jnp.sin(angles)[:, None, :]
    first = tensor[..., :half]
    second = tensor[..., half:]
    return jnp.concatenate([first * cosine - second * sine, second * cosine + first * sine], axis=-1)


def reference(inputs, w_query, w_key, w_value, w_out, chosen):
    group = HEADS // KV_HEADS
    positions = jnp.arange(TOKENS, dtype=jnp.int32)
    queries = rotate(jnp.dot(inputs, w_query, preferred_element_type=jnp.float32).reshape(TOKENS, HEADS, HD), positions).astype(jnp.bfloat16)
    keys = rotate(jnp.dot(inputs, w_key, preferred_element_type=jnp.float32).reshape(TOKENS, KV_HEADS, HD), positions).astype(jnp.bfloat16)
    values = jnp.dot(inputs, w_value, preferred_element_type=jnp.float32).astype(jnp.bfloat16)
    key_blocks = keys.reshape(NBLOCKS, BLK, KV_HEADS, HD)
    value_blocks = values.reshape(NBLOCKS, BLK, KV_HEADS, HD)
    scale = HD ** -0.5

    def one_block(args):
        query_block, listed, index = args
        safe = jnp.maximum(listed, 0)
        near_keys = key_blocks[safe].reshape(SEL * BLK, KV_HEADS, HD).astype(jnp.float32)
        near_values = value_blocks[safe].reshape(SEL * BLK, KV_HEADS, HD).astype(jnp.float32)
        grouped = query_block.reshape(BLK, KV_HEADS, group, HD).astype(jnp.float32)
        score = jnp.einsum('qkgd,skd->kgqs', grouped, near_keys) * scale
        key_pos = (listed[:, None] * BLK + jnp.arange(BLK, dtype=jnp.int32)[None, :]).reshape(-1)
        key_live = jnp.repeat(listed >= 0, BLK)
        query_pos = index * BLK + jnp.arange(BLK, dtype=jnp.int32)
        valid = key_live[None, :] & (key_pos[None, :] <= query_pos[:, None])
        score = jnp.where(valid, score, -jnp.inf)
        top = jnp.max(score, axis=-1)
        weight = jnp.where(valid, jnp.exp(score - top[..., None]), 0.0)
        total = jnp.sum(weight, axis=-1)
        summed = jnp.einsum('kgqs,skd->kgqd', weight, near_values) / total[..., None]
        attended = jnp.transpose(summed, (2, 0, 1, 3)).reshape(BLK, HEADS * HD).astype(jnp.bfloat16)
        log_row = (top + jnp.log(total)).reshape(HEADS, BLK)
        return attended, log_row

    blocks = queries.reshape(NBLOCKS, BLK, HEADS, HD)
    attended, log_rows = lax.map(one_block, (blocks, chosen, jnp.arange(NBLOCKS, dtype=jnp.int32)))
    attended = attended.reshape(TOKENS, HEADS * HD)
    mixed = jnp.dot(attended, w_out, preferred_element_type=jnp.float32).astype(jnp.bfloat16)
    log_total = jnp.transpose(log_rows, (1, 0, 2)).reshape(HEADS, TOKENS)
    return mixed, log_total
```

```python
import functools

import jax
import jax.numpy as jnp
import numpy as np
from jax import lax
from jax.experimental import pallas as pl
from jax.experimental.pallas import tpu as pltpu
from jax.sharding import PartitionSpec as P

HD = 128
BLK = 32
TILE = 128
MESH = pl.DeviceIdType.MESH
F32 = jnp.float32
BF16 = jnp.bfloat16


def iota(shape, dim):
    return lax.broadcasted_iota(jnp.int32, shape, dim)


def kernel(
    peers, tp, x_hbm, wq_hbm, wk_hbm, wv_hbm, wo_hbm, chosen_hbm,
    out, log_total,
    x, wq, wk, wv, wo, chosen, cosine, sine, kv, q, request, pick, stage, far, bias, gathered, acc,
    load_sem, req_send, req_recv, far_send, far_recv,
    ring_send, ring_recv, side_send, side_recv, pass_send, pass_recv,
):
    tokens = x.shape[0]
    heads = wq.shape[1] // HD
    kv_heads = wk.shape[1] // HD
    group = heads // kv_heads
    blocks = tokens // BLK
    count = chosen.shape[0] - 1
    reaches = [1 + k * (peers - 2) // (count - 1) for k in range(count)]
    chips = tp // 2
    tiles = tokens // TILE
    me = lax.axis_index("kv")
    lane = lax.axis_index("tp")
    chip, core = lane // 2, lane % 2
    partner = chip * 2 + 1 - core
    scale = HD ** -0.5

    loads = [
        pltpu.make_async_copy(s, d, load_sem.at[i])
        for i, (s, d) in enumerate(
            [(chosen_hbm, chosen), (x_hbm, x), (wk_hbm, wk), (wv_hbm, wv),
             (wq_hbm, wq), (wo_hbm, wo)]
        )
    ]

    barrier = pltpu.get_barrier_semaphore()
    expected = jnp.int32(chips)
    for d in reaches:
        @pl.when(me >= d)
        def _():
            pl.semaphore_signal(barrier, inc=1, device_id=(me - d, lane), device_id_type=MESH)

        @pl.when(me + d < peers)
        def _():
            pl.semaphore_signal(barrier, inc=1, device_id=(me + d, lane), device_id_type=MESH)

        expected = expected + jnp.where(me >= d, 1, 0) + jnp.where(me + d < peers, 1, 0)
    pl.semaphore_signal(barrier, inc=1, device_id=(me, partner), device_id_type=MESH)
    for step in range(1, chips):
        other = lax.rem(chip + step, chips) * 2 + core
        pl.semaphore_signal(barrier, inc=1, device_id=(me, other), device_id_type=MESH)
    for load in loads[:4]:
        load.start()

    def request_copy(k):
        return pltpu.make_async_remote_copy(
            src_ref=chosen, dst_ref=request.at[k], send_sem=req_send.at[k],
            recv_sem=req_recv.at[k], device_id=(me - reaches[k], lane), device_id_type=MESH,
        )

    def far_copy(k):
        rows = pl.ds(k * BLK, BLK)
        return pltpu.make_async_remote_copy(
            src_ref=stage.at[rows], dst_ref=far.at[rows], send_sem=far_send.at[k],
            recv_sem=far_recv.at[k], device_id=(me + reaches[k], lane), device_id_type=MESH,
        )

    half = HD // 2
    which = iota((1, HD), 1) % half
    inv = jnp.ones((1, HD), F32)
    for j in range(1, half):
        inv = jnp.where(which == j, np.float32(10000.0 ** (-j / half)), inv)
    angle = (me * tokens + iota((tokens, HD), 0)).astype(F32) * inv
    cosine[...] = jnp.cos(angle)
    wave = jnp.sin(angle)
    sine[...] = jnp.where(iota((tokens, HD), 1) < HD // 2, -wave, wave)
    loads[0].wait()
    live = jnp.where(chosen[...] >= 0, 1.0, 0.0).astype(BF16)
    spread = jnp.where(
        iota((count + 1, far.shape[0]), 0) == iota((count + 1, far.shape[0]), 1) // BLK + 1, 1.0, 0.0
    ).astype(BF16)
    rows_of = jnp.where(
        iota((tokens, blocks), 0) // BLK == iota((tokens, blocks), 1), 1.0, 0.0
    ).astype(BF16)
    lists = lax.dot_general(
        rows_of, live, (((1,), (1,)), ((), ())), preferred_element_type=F32
    ).astype(BF16)
    admitted = jnp.dot(lists, spread, preferred_element_type=F32)
    bias[...] = jnp.where(admitted > 0.5, 0.0, -jnp.inf)

    pl.semaphore_wait(barrier, expected)
    for k in range(count):
        @pl.when(me >= reaches[k])
        def _():
            request_copy(k).start()

        @pl.when(me < reaches[k])
        def _():
            far[k * BLK:(k + 1) * BLK, :] = jnp.zeros((BLK, far.shape[1]), BF16)

    if far.shape[0] > count * BLK:
        far[count * BLK:, :] = jnp.zeros((far.shape[0] - count * BLK, far.shape[1]), BF16)

    loads[4].start()
    loads[5].start()

    def project(weights, columns, rows=slice(None)):
        return jnp.dot(x[rows, :], weights[:, columns], preferred_element_type=F32)

    def rotated(t, rows=slice(None)):
        turned = pltpu.roll(t, HD // 2, 1)
        return (t * cosine[rows, :] + turned * sine[rows, :]).astype(BF16)

    loads[1].wait()
    loads[2].wait()
    t = project(wk, slice(0, kv_heads * HD))
    for h in range(kv_heads):
        kv[:, h * HD:(h + 1) * HD] = rotated(t[:, h * HD:(h + 1) * HD])
    loads[3].wait()
    kv[:, kv_heads * HD:] = project(wv, slice(0, kv_heads * HD)).astype(BF16)

    for k in range(count):
        span = slice(k * BLK, (k + 1) * BLK)

        @pl.when(me + reaches[k] < peers)
        def _():
            request_copy(k).wait_recv()
            asked = request[k][k + 1:k + 2, blocks - 1:blocks]
            inner = jnp.maximum(asked - me * blocks, 0) * BLK
            wanted = iota((BLK, tokens), 1) == iota((BLK, tokens), 0) + inner
            pick[span, :] = jnp.where(wanted, 1.0, 0.0).astype(BF16)

        @pl.when(me + reaches[k] >= peers)
        def _():
            pick[span, :] = jnp.zeros((BLK, tokens), BF16)

    stage[...] = jnp.dot(pick[...], kv[...], preferred_element_type=F32).astype(BF16)
    for k in range(count):
        @pl.when(me + reaches[k] < peers)
        def _():
            far_copy(k).start()

    loads[4].wait()

    def make_queries(rows):
        for first in range(0, heads, 2):
            t = project(wq, slice(first * HD, (first + 2) * HD), rows)
            for h in range(2):
                q[rows, (first + h) * HD:(first + h + 1) * HD] = rotated(
                    t[:, h * HD:(h + 1) * HD], rows
                )

    make_queries(slice(0, tokens // 2))

    for k in range(count):
        @pl.when(me >= reaches[k])
        def _():
            request_copy(k).wait_send()
            far_copy(k).wait_recv()

    def side_copy(i):
        rows = pl.ds(pl.multiple_of(i * TILE, TILE), TILE)
        return pltpu.make_async_remote_copy(
            src_ref=gathered.at[lane, rows], dst_ref=gathered.at[lane, rows],
            send_sem=side_send.at[i], recv_sem=side_recv.at[i],
            device_id=(me, partner), device_id_type=MESH,
        )

    def ring_copy(step, i):
        rows = pl.ds(pl.multiple_of(i * TILE, TILE), TILE)
        return pltpu.make_async_remote_copy(
            src_ref=gathered.at[lane, rows], dst_ref=gathered.at[lane, rows],
            send_sem=ring_send.at[step - 1, i], recv_sem=ring_recv.at[step - 1, i],
            device_id=(me, lax.rem(chip + step, chips) * 2 + core), device_id_type=MESH,
        )

    def origin(step):
        return lax.rem(chip - step + chips, chips)

    def pass_copy(step, i):
        rows = pl.ds(pl.multiple_of(i * TILE, TILE), TILE)
        slot = origin(step) * 2 + core
        return pltpu.make_async_remote_copy(
            src_ref=gathered.at[slot, rows], dst_ref=gathered.at[slot, rows],
            send_sem=pass_send.at[step - 1, i], recv_sem=pass_recv.at[step - 1, i],
            device_id=(me, partner), device_id_type=MESH,
        )

    row_id, col_id = iota((TILE, TILE), 0), iota((TILE, TILE), 1)
    near_bias = jnp.where((row_id // BLK == col_id // BLK) & (col_id <= row_id), 0.0, -jnp.inf)
    contract = (((1,), (1,)), ((), ()))

    def attend(i, carry):
        rows = pl.ds(pl.multiple_of(i * TILE, TILE), TILE)
        far_bias = bias[rows, :]
        logs = jnp.zeros((TILE, TILE), F32)
        for h in range(heads):
            g = h // group
            keys = slice(g * HD, (g + 1) * HD)
            vals = slice((kv_heads + g) * HD, (kv_heads + g + 1) * HD)
            qh = q[rows, h * HD:(h + 1) * HD]
            s_far = lax.dot_general(qh, far[:, keys], contract, preferred_element_type=F32)
            s_near = lax.dot_general(qh, kv[rows, keys], contract, preferred_element_type=F32)
            s_far = s_far * scale + far_bias
            s_near = s_near * scale + near_bias
            top = jnp.maximum(
                jnp.max(s_far, axis=1, keepdims=True), jnp.max(s_near, axis=1, keepdims=True)
            )
            p_far = jnp.exp(s_far - top)
            p_near = jnp.exp(s_near - top)
            total = jnp.sum(p_far, axis=1, keepdims=True) + jnp.sum(p_near, axis=1, keepdims=True)
            summed = jnp.dot(p_far.astype(BF16), far[:, vals], preferred_element_type=F32)
            summed += jnp.dot(p_near.astype(BF16), kv[rows, vals], preferred_element_type=F32)
            gathered[lane, rows, h * HD:(h + 1) * HD] = (summed / total).astype(BF16)
            logs = jnp.where(col_id == h, top + jnp.log(total), logs)
        log_total[:, rows] = jnp.transpose(logs)[:heads]
        for step in range(1, chips):
            ring_copy(step, i).start()
        side_copy(i).start()
        return carry

    lax.fori_loop(0, tiles // 2, attend, 0)
    make_queries(slice(tokens // 2, tokens))
    lax.fori_loop(tiles // 2, tiles, attend, 0)

    width = heads * HD

    def term(slot, rows):
        return jnp.dot(
            gathered[slot, rows, :], wo[pl.ds(pl.multiple_of(slot * width, width), width), :],
            preferred_element_type=F32,
        )

    everything = pl.ds(0, tokens)
    loads[5].wait()
    acc[...] = term(lane, everything)

    def take_side(i, carry):
        side_copy(i).wait_recv()
        return carry

    lax.fori_loop(0, tiles, take_side, 0)
    acc[...] += term(partner, everything)

    def finish(i, carry):
        rows = pl.ds(pl.multiple_of(i * TILE, TILE), TILE)
        total = acc[rows, :]
        for step in range(1, chips):
            ring_copy(step, i).wait_recv()
            pass_copy(step, i).start()
            total += term(origin(step) * 2 + core, rows)
        for step in range(1, chips):
            pass_copy(step, i).wait_recv()
            total += term(origin(step) * 2 + 1 - core, rows)
        out[rows, :] = total.astype(BF16)
        return carry

    lax.fori_loop(0, tiles, finish, 0)

    def drain(i, carry):
        side_copy(i).wait_send()
        for step in range(1, chips):
            ring_copy(step, i).wait_send()
            pass_copy(step, i).wait_send()
        return carry

    lax.fori_loop(0, tiles, drain, 0)
    for k in range(count):
        @pl.when(me + reaches[k] < peers)
        def _():
            far_copy(k).wait_send()


def local(peers, tp, inputs, w_query, w_key, w_value, w_out, chosen):
    tokens, _ = inputs.shape
    heads = w_query.shape[1] // HD
    kv_heads = w_key.shape[1] // HD
    chosen = chosen.T
    count = chosen.shape[0] - 1
    far_rows = -(-count * BLK // TILE) * TILE
    tiles = tokens // TILE
    chips = tp // 2
    hbm = pl.BlockSpec(memory_space=pltpu.HBM)
    vmem = pl.BlockSpec(memory_space=pltpu.VMEM)
    dma = pltpu.SemaphoreType.DMA
    shapes = (
        pltpu.VMEM((tokens, w_out.shape[1]), BF16),
        pltpu.VMEM((heads, tokens), F32),
    )
    return pl.pallas_call(
        functools.partial(kernel, peers, tp),
        out_shape=shapes,
        in_specs=[hbm] * 6,
        out_specs=(vmem, vmem),
        scratch_shapes=[
            pltpu.VMEM(inputs.shape, BF16),
            pltpu.VMEM(w_query.shape, BF16),
            pltpu.VMEM(w_key.shape, BF16),
            pltpu.VMEM(w_value.shape, BF16),
            pltpu.VMEM(w_out.shape, BF16),
            pltpu.VMEM(chosen.shape, jnp.int32),
            pltpu.VMEM((tokens, HD), F32),
            pltpu.VMEM((tokens, HD), F32),
            pltpu.VMEM((tokens, 2 * kv_heads * HD), BF16),
            pltpu.VMEM((tokens, heads * HD), BF16),
            pltpu.VMEM((count,) + chosen.shape, jnp.int32),
            pltpu.VMEM((count * BLK, tokens), BF16),
            pltpu.VMEM((count * BLK, 2 * kv_heads * HD), BF16),
            pltpu.VMEM((far_rows, 2 * kv_heads * HD), BF16),
            pltpu.VMEM((tokens, far_rows), F32),
            pltpu.VMEM((tp, tokens, heads * HD), BF16),
            pltpu.VMEM((tokens, w_out.shape[1]), F32),
            dma((6,)),
            dma((count,)), dma((count,)), dma((count,)), dma((count,)),
            dma((chips - 1, tiles)), dma((chips - 1, tiles)),
            dma((tiles,)), dma((tiles,)),
            dma((chips - 1, tiles)), dma((chips - 1, tiles)),
        ],
        compiler_params=pltpu.CompilerParams(
            collective_id=0, has_side_effects=True, vmem_limit_bytes=66_400_000
        ),
    )(inputs, w_query, w_key, w_value, w_out, chosen)


def solution(mesh):
    placed = (
        P("kv", None),
        P(None, "tp"),
        P(None, "tp"),
        P(None, "tp"),
        P(None, "tp"),
        P("kv", None),
    )
    return jax.shard_map(
        functools.partial(local, mesh.shape["kv"], mesh.shape["tp"]),
        mesh=mesh, in_specs=placed, out_specs=(P("kv", "tp"), P("tp", "kv")), check_vma=False,
    )
```

```python
import contextlib
import functools

import jax
import jax.numpy as jnp
import numpy as np
from jax import lax
from jax.experimental import pallas as pl
from jax.experimental.pallas import tpu as pltpu
from jax.sharding import PartitionSpec as P

HD = 128
BLK = 32
TILE = 128
MESH = pl.DeviceIdType.MESH
F32 = jnp.float32
BF16 = jnp.bfloat16
LOG2E = 1.4426950408889634


def scope(name):
    return contextlib.nullcontext()


def iota(shape, dim):
    return lax.broadcasted_iota(jnp.int32, shape, dim)


def kernel(
    peers, tp, x_hbm, wq_hbm, wk_hbm, wv_hbm, wo_hbm, chosen_hbm,
    out, log_total,
    x, wq, wkv, wo, chosen, cosine, sine, kv, q, request, stage, far, bias, gathered, acc,
    near_o, near_m,
    load_sem, req_send, req_recv, far_send, far_recv,
    ring_send, ring_recv, side_send, side_recv, pass_send, pass_recv,
):
    tokens = x.shape[0]
    heads = wq.shape[1] // HD
    kv_heads = wkv.shape[1] // (2 * HD)
    kv_wide = kv_heads * HD
    group = heads // kv_heads
    wide = group * HD
    blocks = tokens // BLK
    count = chosen.shape[0] - 1
    reaches = [1 + k * (peers - 2) // (count - 1) for k in range(count)]
    chips = tp // 2
    tiles = tokens // TILE
    me = lax.axis_index("kv")
    lane = lax.axis_index("tp")
    chip, core = lane // 2, lane % 2
    partner = chip * 2 + 1 - core
    scale = HD ** -0.5
    factor = scale * LOG2E

    loads = [
        pltpu.make_async_copy(s, d, load_sem.at[i])
        for i, (s, d) in enumerate(
            [(chosen_hbm, chosen), (x_hbm, x), (wk_hbm, wkv.at[:, pl.ds(0, kv_wide)]),
             (wv_hbm, wkv.at[:, pl.ds(kv_wide, kv_wide)]), (wq_hbm, wq), (wo_hbm, wo)]
        )
    ]
    barrier = pltpu.get_barrier_semaphore()
    pl.semaphore_signal(barrier, inc=1, device_id=(me, partner), device_id_type=MESH)
    for step in range(1, chips):
        other = lax.rem(chip + step, chips) * 2 + core
        pl.semaphore_signal(barrier, inc=1, device_id=(me, other), device_id_type=MESH)
    expected = jnp.int32(chips)
    for d in reaches:
        @pl.when(me + d < peers)
        def _():
            pl.semaphore_signal(barrier, inc=1, device_id=(me + d, lane), device_id_type=MESH)

        expected = expected + jnp.where(me >= d, 1, 0)
    for load in loads[:4]:
        load.start()

    def request_copy(k):
        return pltpu.make_async_remote_copy(
            src_ref=chosen, dst_ref=request.at[k], send_sem=req_send.at[k],
            recv_sem=req_recv.at[k], device_id=(me - reaches[k], lane), device_id_type=MESH,
        )

    def far_copy(k, g):
        rows, cols = pl.ds(k * BLK, BLK), pl.ds(g * 2 * HD, 2 * HD)
        return pltpu.make_async_remote_copy(
            src_ref=stage.at[rows, cols], dst_ref=far.at[rows, cols], send_sem=far_send.at[k, g],
            recv_sem=far_recv.at[k, g], device_id=(me + reaches[k], lane), device_id_type=MESH,
        )

    with scope("trig"):
        half = HD // 2
        fold = tokens // 2
        which = iota((1, HD), 1) % half
        inv = jnp.ones((1, HD), F32)
        for j in range(1, half):
            inv = jnp.where(which == j, np.float32(10000.0 ** (-j / half)), inv)
        low = iota((fold, HD), 1) < half
        position = me * tokens + iota((fold, HD), 0) + jnp.where(low, 0, fold)
        angle = position.astype(F32) * inv
        wave = jnp.cos(angle)
        turned = pltpu.roll(wave, half, 1)
        cosine[:fold, :] = jnp.where(low, wave, turned)
        cosine[fold:, :] = jnp.where(low, turned, wave)
        wave = jnp.sin(angle)
        turned = pltpu.roll(wave, half, 1)
        sine[:fold, :] = jnp.where(low, -wave, turned)
        sine[fold:, :] = jnp.where(low, -turned, wave)

    with scope("barr"):
        loads[0].wait()
        pl.semaphore_wait(barrier, expected)
    for k in range(count):
        @pl.when(me >= reaches[k])
        def _():
            request_copy(k).start()

        @pl.when(me < reaches[k])
        def _():
            far[k * BLK:(k + 1) * BLK, :] = jnp.zeros((BLK, far.shape[1]), BF16)

    if far.shape[0] > count * BLK:
        far[count * BLK:, :] = jnp.zeros((far.shape[0] - count * BLK, far.shape[1]), BF16)

    with scope("bias"):
        live = jnp.where(chosen[...] >= 0, 1.0, 0.0).astype(BF16)
        spread = jnp.where(
            iota((count + 1, far.shape[0]), 0) == iota((count + 1, far.shape[0]), 1) // BLK + 1, 1.0, 0.0
        ).astype(BF16)
        rows_of = jnp.where(
            iota((tokens, blocks), 0) // BLK == iota((tokens, blocks), 1), 1.0, 0.0
        ).astype(BF16)
        lists = lax.dot_general(
            rows_of, live, (((1,), (1,)), ((), ())), preferred_element_type=F32
        ).astype(BF16)
        admitted = jnp.dot(lists, spread, preferred_element_type=F32)
        bias[...] = jnp.where(admitted > 0.5, 0.0, -jnp.inf)

    def rotated(t, rows=slice(None)):
        turned = pltpu.roll(t, HD // 2, 1)
        return (t * cosine[rows, :] + turned * sine[rows, :]).astype(BF16)

    with scope("waitx"):
        loads[1].wait()
        loads[2].wait()
        loads[3].wait()
    loads[4].start()
    with scope("kvproj"):
        t = jnp.dot(x[...], wkv[...], preferred_element_type=F32)
        for h in range(kv_heads):
            at = 2 * h * HD
            kv[:, at:at + HD] = rotated(t[:, h * HD:(h + 1) * HD])
            kv[:, at + HD:at + 2 * HD] = t[:, kv_wide + h * HD:kv_wide + (h + 1) * HD].astype(BF16)
    loads[5].start()

    def serve(k):
        @pl.when(me + reaches[k] < peers)
        def _():
            request_copy(k).wait_recv()
            asked = jnp.broadcast_to(request[k, k + 1:k + 2, blocks - 1:blocks], (BLK, HD))
            chunks = [jnp.zeros((BLK, HD), BF16)] * (2 * kv_heads)
            for b in range(blocks):
                wanted = jnp.where(asked == me * blocks + b, 1.0, 0.0).astype(BF16)
                for c in range(2 * kv_heads):
                    chunks[c] += wanted * kv[b * BLK:(b + 1) * BLK, c * HD:(c + 1) * HD]
            for c in range(2 * kv_heads):
                stage[k * BLK:(k + 1) * BLK, c * HD:(c + 1) * HD] = chunks[c]
            far_copy(k, 0).start()

    def follow(k):
        @pl.when(me + reaches[k] < peers)
        def _():
            for g in range(1, kv_heads):
                far_copy(k, g).start()

    contract = (((1,), (1,)), ((), ()))
    ones = jnp.ones((TILE, HD), BF16)

    def stacked(i, g):
        rows = slice(i * TILE, (i + 1) * TILE)
        return jnp.concatenate(
            [q[rows, h * HD:(h + 1) * HD] for h in range(g * group, (g + 1) * group)], axis=0
        )

    def near(several):
        pairs = [(i, g) for i in several for g in range(kv_heads)]
        row_id, col_id = iota((TILE, TILE), 0), iota((TILE, TILE), 1)
        seen = (row_id // BLK == col_id // BLK) & (col_id <= row_id)
        near_bias = jnp.where(seen, 0.0, -jnp.inf)
        near_bias = jnp.concatenate([near_bias] * group, axis=0)
        scores = []
        for i, g in pairs:
            keys = kv[i * TILE:(i + 1) * TILE, 2 * g * HD:(2 * g + 1) * HD]
            scores.append(lax.dot_general(stacked(i, g), keys, contract, preferred_element_type=F32))
        scores = [s + near_bias for s in scores]
        tops = [jnp.max(s, axis=1, keepdims=True) for s in scores]
        weights = [jnp.exp2((s - top) * factor).astype(BF16) for s, top in zip(scores, tops)]
        for (i, g), p, top in zip(pairs, weights, tops):
            at = (2 * g + 1) * HD
            vals = jnp.concatenate([kv[i * TILE:(i + 1) * TILE, at:at + HD], ones], axis=1)
            near_o[i, g] = jnp.dot(p, vals, preferred_element_type=F32)
            near_m[i, g] = jnp.broadcast_to(top, (group * TILE, HD))

    early = me >= reaches[0]

    def serve_if(when, some, after=()):
        @pl.when(when)
        def _():
            for k in some:
                if k < count:
                    serve(k)
            for k in after:
                if k < count:
                    follow(k)

    with scope("serve1"):
        serve_if(early, (0, 1))
    with scope("q"):
        loads[4].wait()
        t = jnp.dot(x[...], wq[...], preferred_element_type=F32)
        for h in range(heads):
            q[:, h * HD:(h + 1) * HD] = rotated(t[:, h * HD:(h + 1) * HD])
    with scope("serve2"):
        serve_if(early, (2, 3, 4), (0, 1))
    with scope("near1"):
        near(range(0, tiles // 2))
    with scope("serve3"):
        serve_if(early, (5,), (2, 3, 4))
    with scope("near2"):
        near(range(tiles // 2, tiles))
    with scope("serve4"):
        serve_if(early, range(6, count), range(5, count))
        serve_if(jnp.logical_not(early), (0, 1, 2))

    def await_far(g):
        for k in range(count):
            @pl.when(me >= reaches[k])
            def _():
                far_copy(k, g).wait_recv()

    def side_copy(i, g):
        rows = pl.ds(pl.multiple_of(i * TILE, TILE), TILE)
        cols = pl.ds(g * wide, wide)
        return pltpu.make_async_remote_copy(
            src_ref=gathered.at[lane, rows, cols], dst_ref=gathered.at[lane, rows, cols],
            send_sem=side_send.at[i, g], recv_sem=side_recv.at[i, g],
            device_id=(me, partner), device_id_type=MESH,
        )

    def ring_copy(step, i, g):
        rows = pl.ds(pl.multiple_of(i * TILE, TILE), TILE)
        cols = pl.ds(g * wide, wide)
        return pltpu.make_async_remote_copy(
            src_ref=gathered.at[lane, rows, cols], dst_ref=gathered.at[lane, rows, cols],
            send_sem=ring_send.at[step - 1, i, g], recv_sem=ring_recv.at[step - 1, i, g],
            device_id=(me, lax.rem(chip + step, chips) * 2 + core), device_id_type=MESH,
        )

    def origin(step):
        return lax.rem(chip - step + chips, chips)

    def pass_copy(step, i, g):
        rows = pl.ds(pl.multiple_of(i * TILE, TILE), TILE)
        cols = pl.ds(g * wide, wide)
        slot = origin(step) * 2 + core
        return pltpu.make_async_remote_copy(
            src_ref=gathered.at[slot, rows, cols], dst_ref=gathered.at[slot, rows, cols],
            send_sem=pass_send.at[step - 1, i, g], recv_sem=pass_recv.at[step - 1, i, g],
            device_id=(me, partner), device_id_type=MESH,
        )

    def attend(several, g):
        keys = far[:, 2 * g * HD:(2 * g + 1) * HD]
        vals = jnp.concatenate(
            [far[:, (2 * g + 1) * HD:(2 * g + 2) * HD], jnp.ones((far.shape[0], HD), BF16)], axis=1
        )
        scores = []
        for i in several:
            mask = jnp.concatenate([bias[i * TILE:(i + 1) * TILE, :]] * group, axis=0)
            s = lax.dot_general(stacked(i, g), keys, contract, preferred_element_type=F32)
            scores.append(s + mask)
        tops = [
            jnp.maximum(near_m[i, g], jnp.max(s, axis=1, keepdims=True))
            for i, s in zip(several, scores)
        ]
        weights = [
            jnp.concatenate([
                jnp.exp2((s[:, c:c + HD] - top) * factor).astype(BF16)
                for c in range(0, far.shape[0], HD)
            ], axis=1)
            for s, top in zip(scores, tops)
        ]
        for i, p, top in zip(several, weights, tops):
            rows = slice(i * TILE, (i + 1) * TILE)
            summed = jnp.dot(p, vals, preferred_element_type=F32)
            fade = jnp.exp2((near_m[i, g] - top) * factor)
            total = summed[:, HD:] + fade * near_o[i, g, :, HD:]
            done = summed[:, :HD] + fade * near_o[i, g, :, :HD]
            done = (done * (1.0 / total)).astype(BF16)
            for h in range(group):
                at = (g * group + h) * HD
                gathered[lane, rows, at:at + HD] = done[h * TILE:(h + 1) * TILE]
            for step in range(1, chips):
                ring_copy(step, i, g).start()
            side_copy(i, g).start()
            near_m[i, g] = top * scale + jnp.log(total)

    for g in range(kv_heads):
        with scope("waitfar"):
            await_far(g)
        for first in range(0, tiles, 2):
            with scope("att"):
                attend(range(first, first + 2), g)
            if g == 0 and first == 0:
                with scope("serve5"):
                    serve_if(jnp.logical_not(early), range(3, count), range(count))

    def logs():
        lane_id = iota((TILE, TILE), 1)
        for i in range(tiles):
            rows = jnp.zeros((TILE, TILE), F32)
            for h in range(heads):
                part = slice(h % group * TILE, (h % group + 1) * TILE)
                rows = jnp.where(lane_id == h, near_m[i, h // group, part, :], rows)
            log_total[:, i * TILE:(i + 1) * TILE] = jnp.transpose(rows)[:heads]

    width = heads * HD

    def term(slot, rows):
        return jnp.dot(
            gathered[slot, rows, :], wo[pl.ds(pl.multiple_of(slot * width, width), width), :],
            preferred_element_type=F32,
        )

    everything = pl.ds(0, tokens)
    with scope("ownterm"):
        loads[5].wait()
        acc[...] = term(lane, everything)

    with scope("logs"):
        logs()

    def part(slot, i, g):
        at = pl.multiple_of(slot * width + g * wide, wide)
        return jnp.dot(
            gathered[slot, i * TILE:(i + 1) * TILE, g * wide:(g + 1) * wide], wo[pl.ds(at, wide), :],
            preferred_element_type=F32,
        )

    with scope("waitside"):
        for i in range(tiles):
            for g in range(kv_heads):
                side_copy(i, g).wait_recv()
    with scope("sideterm"):
        acc[...] += term(partner, everything)

    pieces = [(i, g) for g in range(kv_heads) for i in range(tiles)]

    def finish(i, g):
        rows = slice(i * TILE, (i + 1) * TILE)
        with scope("waitpass"):
            for step in range(1, chips):
                pass_copy(step, i, g).wait_recv()
        total = acc[rows, :]
        for step in range(1, chips):
            total += part(origin(step) * 2 + 1 - core, i, g)
        if g == kv_heads - 1:
            out[rows, :] = total.astype(BF16)
        else:
            acc[rows, :] = total

    for n, (i, g) in enumerate(pieces):
        rows = slice(i * TILE, (i + 1) * TILE)
        with scope("waitring"):
            for step in range(1, chips):
                ring_copy(step, i, g).wait_recv()
                pass_copy(step, i, g).start()
        total = acc[rows, :]
        for step in range(1, chips):
            total += part(origin(step) * 2 + core, i, g)
        acc[rows, :] = total
        if n:
            finish(*pieces[n - 1])
    finish(*pieces[-1])

    def drain(i, carry):
        for g in range(kv_heads):
            side_copy(i, g).wait_send()
            for step in range(1, chips):
                ring_copy(step, i, g).wait_send()
                pass_copy(step, i, g).wait_send()
        return carry

    with scope("drain"):
        lax.fori_loop(0, tiles, drain, 0)
        for k in range(count):
            @pl.when(me >= reaches[k])
            def _():
                request_copy(k).wait_send()

            @pl.when(me + reaches[k] < peers)
            def _():
                for g in range(kv_heads):
                    far_copy(k, g).wait_send()


def local(peers, tp, inputs, w_query, w_key, w_value, w_out, chosen):
    tokens, _ = inputs.shape
    heads = w_query.shape[1] // HD
    kv_heads = w_key.shape[1] // HD
    chosen = chosen.T
    count = chosen.shape[0] - 1
    far_rows = -(-count * BLK // TILE) * TILE
    tiles = tokens // TILE
    chips = tp // 2
    hbm = pl.BlockSpec(memory_space=pltpu.HBM)
    vmem = pl.BlockSpec(memory_space=pltpu.VMEM)
    dma = pltpu.SemaphoreType.DMA
    shapes = (
        pltpu.VMEM((tokens, w_out.shape[1]), BF16),
        pltpu.VMEM((heads, tokens), F32),
    )
    return pl.pallas_call(
        functools.partial(kernel, peers, tp),
        out_shape=shapes,
        in_specs=[hbm] * 6,
        out_specs=(vmem, vmem),
        scratch_shapes=[
            pltpu.VMEM(inputs.shape, BF16),
            pltpu.VMEM(w_query.shape, BF16),
            pltpu.VMEM((w_key.shape[0], 2 * w_key.shape[1]), BF16),
            pltpu.VMEM(w_out.shape, BF16),
            pltpu.VMEM(chosen.shape, jnp.int32),
            pltpu.VMEM((tokens, HD), F32),
            pltpu.VMEM((tokens, HD), F32),
            pltpu.VMEM((tokens, 2 * kv_heads * HD), BF16),
            pltpu.VMEM((tokens, heads * HD), BF16),
            pltpu.VMEM((count,) + chosen.shape, jnp.int32),
            pltpu.VMEM((count * BLK, 2 * kv_heads * HD), BF16),
            pltpu.VMEM((far_rows, 2 * kv_heads * HD), BF16),
            pltpu.VMEM((tokens, far_rows), F32),
            pltpu.VMEM((tp, tokens, heads * HD), BF16),
            pltpu.VMEM((tokens, w_out.shape[1]), F32),
            pltpu.VMEM((tiles, kv_heads, heads // kv_heads * TILE, 2 * HD), F32),
            pltpu.VMEM((tiles, kv_heads, heads // kv_heads * TILE, HD), F32),
            dma((6,)),
            dma((count,)), dma((count,)), dma((count, kv_heads)), dma((count, kv_heads)),
            dma((chips - 1, tiles, kv_heads)), dma((chips - 1, tiles, kv_heads)),
            dma((tiles, kv_heads)), dma((tiles, kv_heads)),
            dma((chips - 1, tiles, kv_heads)), dma((chips - 1, tiles, kv_heads)),
        ],
        compiler_params=pltpu.CompilerParams(
            collective_id=0, has_side_effects=True, vmem_limit_bytes=66_400_000
        ),
    )(inputs, w_query, w_key, w_value, w_out, chosen)


def solution(mesh):
    placed = (
        P("kv", None),
        P(None, "tp"),
        P(None, "tp"),
        P(None, "tp"),
        P(None, "tp"),
        P("kv", None),
    )
    return jax.shard_map(
        functools.partial(local, mesh.shape["kv"], mesh.shape["tp"]),
        mesh=mesh, in_specs=placed, out_specs=(P("kv", "tp"), P("tp", "kv")), check_vma=False,
    )
```
